32 devices in a mesh: sp: 8 (over z, x), tp: 4 (over y, core).
Axes of the slice: x: 2, y: 2, z: 4, core: 2. Of those that a mesh axis runs over, the one named last changes fastest.
Arguments:
- queries: bfloat16 [5120, 1024], P('sp', 'tp'), may hold values from -6 to 6
- key_head_rows: bfloat16 [5120, 1024], P('sp', 'tp'), may hold values from -6 to 6
- value_head_rows: bfloat16 [5120, 2048], P('sp', 'tp'), may hold values from -6 to 6
- output_gate_preact: bfloat16 [5120, 2048], P('sp', 'tp'), may hold values from -6 to 6
- log_input_gate: float32 [16, 5120], P('tp', 'sp'), may hold values from -4 to 300
- forget_gate_preact: float32 [16, 5120], P('tp', 'sp')
- extra_log_decay: float32 [16, 5120], P('tp', 'sp'), may hold values from -2.1 to 0
- head_norm_gain: float32 [2048], P('tp'), may hold values from 0.1 to 1.9
- residual: bfloat16 [5120, 2048], P(('sp', 'tp')), may hold values from -6 to 6
- cell_output_weight: bfloat16 [2048, 2048], P('tp'), may hold values from -0.25 to 0.25
- feedforward_norm_gain: float32 [2048], replicated, may hold values from 0.1 to 1.9
- gate_projection_weight: bfloat16 [2048, 5632], P('sp', 'tp'), may hold values from -0.125 to 0.125
- up_projection_weight: bfloat16 [2048, 5632], P('sp', 'tp'), may hold values from -0.125 to 0.125
- down_projection_weight: bfloat16 [5632, 2048], P('tp', 'sp'), may hold values from -0.109375 to 0.109375
Outputs:
- layer_out: bfloat16 [5120, 2048], P(('sp', 'tp'))
The draws below stay inside these ranges and needn't reach their ends.
All inputs are finite; a program needn't handle non-finite values.
Results may differ from the reference program's by a relative error of at most 0.015.
Values may be sent and summed in bfloat16 or wider, within the bound.
A program may use at most 128 MiB of HBM per device.

```python
import jax
import jax.numpy as jnp
from jax import lax

D = 2048
HEADS = 16
DQK = 64
DV = 128
FF = 5632
BLOCK = 128
TOK_DEV = 640
TOKENS = 5120
HV = 2048
N_TP = 4


def draw_log_input_gate(key, part):
    base_key = jax.random.fold_in(key, 0)
    return jnp.clip(jax.random.normal(base_key, (HEADS, TOKENS), jnp.float32), -4.0, 4.0)


def draw_forget_gate_preact(key, part):
    kind_key, block_key, noise_key = jax.random.split(key, 3)
    fast_share = 0.5
    fast_heads = jax.random.uniform(kind_key, (HEADS, 1), jnp.float32) < fast_share
    base_rate = jnp.where(fast_heads, 1.0 / 40.0, 0.5 / TOKENS)
    span_scale = jax.random.uniform(block_key, (HEADS, TOKENS // TOK_DEV), jnp.float32, 0.35, 1.0)
    span_scale = jnp.repeat(span_scale, TOK_DEV, axis=1)
    jitter = jnp.exp(0.7 * jnp.clip(jax.random.normal(noise_key, (HEADS, TOKENS), jnp.float32), -3.0, 3.0))
    decay_rate = base_rate * span_scale * jitter
    return -jnp.log(jnp.expm1(decay_rate))


def draw_extra_log_decay(key, part):
    spot_key, size_key = jax.random.split(key, 2)
    spot_list = jax.random.randint(spot_key, (HEADS, 3), 0, TOKENS)
    drop_sizes = jax.random.uniform(size_key, (HEADS, 3, 1), jnp.float32, 0.22, 0.69)
    hit_mask = jnp.arange(TOKENS)[None, None, :] == spot_list[:, :, None]
    return -jnp.sum(jnp.where(hit_mask, drop_sizes, 0.0), axis=1)


def block_scale(key, shape, shards, least, top_value):
    def one(dim, parts):
        draws = jax.random.uniform(jax.random.fold_in(jax.random.fold_in(key, 6), dim), (parts,), jnp.float32, least / len(shards), top_value / len(shards))
        return jnp.repeat(jnp.exp(draws), shape[dim] // parts).reshape((-1,) + (1,) * (len(shape) - dim - 1))

    factor_of = one(*shards[0])
    for cut in shards[1:]:
        factor_of = factor_of * one(*cut)
    return factor_of


def noise(own_key, shape, scale, most, cuts=(), dtype=jnp.bfloat16):
    result = scale * jax.random.normal(own_key, shape, jnp.float32)
    if cuts:
        result = result * block_scale(own_key, shape, cuts, -0.22, 0.18)
    return jnp.clip(result, -most, most).astype(dtype)


def setup_inputs(seed: int = 0) -> dict:
    key_of = jax.random.split(jax.random.key(seed), 15)
    queries = noise(key_of[0], (TOKENS, HEADS * DQK), 1.0, 6.0, ((0, 8), (1, 4)))
    key_head_rows = noise(key_of[1], (TOKENS, HEADS * DQK), 1.0, 6.0, ((0, 8), (1, 4)))
    value_head_rows = noise(key_of[2], (TOKENS, HV), 1.0, 6.0, ((0, 8), (1, 4)))
    output_gate_preact = noise(key_of[3], (TOKENS, HV), 1.0, 6.0, ((0, 8), (1, 4)))
    log_input_gate = draw_log_input_gate(jax.random.fold_in(key_of[14], 71), 0)
    forget_gate_preact = draw_forget_gate_preact(jax.random.fold_in(key_of[14], 71), 0)
    extra_log_decay = draw_extra_log_decay(jax.random.fold_in(key_of[14], 71), 0)
    head_norm_gain = jnp.clip(1.0 + 0.18 * jax.random.normal(key_of[7], (HV,), jnp.float32), 0.1, 1.9)
    residual = noise(key_of[8], (TOKENS, D), 1.0, 6.0, ((0, 32),))
    cell_output_weight = noise(key_of[9], (HV, D), (HV // 4) ** -0.5, 0.25, ((0, 4),))
    feedforward_norm_gain = jnp.clip(1.0 + 0.18 * jax.random.normal(key_of[10], (D,), jnp.float32), 0.1, 1.9)
    gate_projection_weight = noise(key_of[11], (D, FF), D ** -0.5, 0.125, ((0, 8), (1, 4)))
    up_projection_weight = noise(key_of[12], (D, FF), D ** -0.5, 0.125, ((0, 8), (1, 4)))
    down_projection_weight = noise(key_of[13], (FF, D), (FF // 2) ** -0.5, 0.109375, ((0, 4), (1, 8)))
    return {"queries": queries, "key_head_rows": key_head_rows, "value_head_rows": value_head_rows, "output_gate_preact": output_gate_preact, "log_input_gate": log_input_gate, "forget_gate_preact": forget_gate_preact, "extra_log_decay": extra_log_decay, "head_norm_gain": head_norm_gain, "residual": residual, "cell_output_weight": cell_output_weight, "feedforward_norm_gain": feedforward_norm_gain, "gate_projection_weight": gate_projection_weight, "up_projection_weight": up_projection_weight, "down_projection_weight": down_projection_weight}


epsilon = 1e-06
lowest = -1e+30

def merge_states(earlier, later):
    state_one, top_one, total_one = earlier
    state_two, top_two, total_two = later
    top_new = jnp.maximum(total_two + top_one, top_two)
    scale_one = jnp.exp(total_two + top_one - top_new)
    scale_two = jnp.exp(top_two - top_new)
    state_new = scale_one[..., None, None] * state_one + scale_two[..., None, None] * state_two
    return (state_new, top_new, total_one + total_two)

def block_parts(key_block, value_block, gate_block, forget_block):
    running = jnp.cumsum(forget_block, axis=-1)
    totals = running[..., -1]
    to_end = totals[..., None] - running + gate_block
    top_block = lax.optimization_barrier(jnp.max(to_end, axis=-1))
    factor = jnp.exp(to_end - top_block[..., None]) * DQK ** (-0.5)
    weighted = (key_block.astype(jnp.float32) * factor[..., None]).astype(jnp.bfloat16)
    states = jnp.einsum('nhsd,nhse->nhde', weighted.astype(jnp.float32), value_block.astype(jnp.float32))
    return (running, (states, top_block, totals))

def block_output(query_block, key_block, value_block, gate_block, running, carried_state, carried_top):
    length = query_block.shape[-2]
    scores = jnp.einsum('nhtd,nhsd->nhts', query_block.astype(jnp.float32), key_block.astype(jnp.float32)) * DQK ** (-0.5)
    log_decay = running[..., :, None] - running[..., None, :] + gate_block[..., None, :]
    causal = jnp.arange(length)[:, None] >= jnp.arange(length)[None, :]
    log_decay = jnp.where(causal, log_decay, -jnp.inf)
    carried = running + carried_top[..., None]
    row_top = jnp.maximum(carried, lax.optimization_barrier(jnp.max(log_decay, axis=-1)))
    weights = (scores * jnp.exp(log_decay - row_top[..., None])).astype(jnp.bfloat16)
    within = jnp.einsum('nhts,nhse->nhte', weights.astype(jnp.float32), value_block.astype(jnp.float32))
    across = jnp.einsum('nhtd,nhde->nhte', query_block.astype(jnp.float32), carried_state, precision=lax.Precision.HIGHEST)
    return jnp.exp(carried - row_top)[..., None] * across + within

def grouped_product(left, right, groups):
    columns = left.shape[1] // groups
    summed = jnp.zeros((left.shape[0], right.shape[1]), jnp.float32)
    for member in range(groups):
        product = jnp.dot(left[:, member * columns:(member + 1) * columns], right[member * columns:(member + 1) * columns], preferred_element_type=jnp.float32)
        rounded = lax.optimization_barrier(product.astype(jnp.bfloat16))
        summed = summed + rounded.astype(jnp.float32)
    return summed

def reference(queries, key_head_rows, value_head_rows, output_gate_preact, log_input_gate, forget_gate_preact, extra_log_decay, head_norm_gain, residual, cell_output_weight, feedforward_norm_gain, gate_projection_weight, up_projection_weight, down_projection_weight):
    blocks = TOKENS // BLOCK

    def split_heads(matrix, head_size):
        return matrix.reshape(blocks, BLOCK, HEADS, head_size).transpose(0, 2, 1, 3)

    def split_gate_parts(gates):
        return gates.reshape(HEADS, blocks, BLOCK).transpose(1, 0, 2)
    log_forget_gate = jax.nn.log_sigmoid(forget_gate_preact) + extra_log_decay
    inputs = (split_heads(queries, DQK), split_heads(key_head_rows, DQK), split_heads(value_head_rows, DV), split_gate_parts(log_input_gate), split_gate_parts(log_forget_gate))

    def advance(history, segment):
        query_block, key_block, value_block, gate_block, forget_block = [member[None] for member in segment]
        running, summary = block_parts(key_block, value_block, gate_block, forget_block)
        numerator = block_output(query_block, key_block, value_block, gate_block, running, history[0][None], history[1][None])
        history = merge_states(history, tuple((member[0] for member in summary)))
        return (history, numerator[0])
    initial = (jnp.zeros((HEADS, DQK, DV), jnp.float32), jnp.full((HEADS,), lowest, jnp.float32), jnp.zeros((HEADS,), jnp.float32))
    _, numerators = lax.scan(advance, initial, inputs)
    numerators = numerators.transpose(0, 2, 1, 3).reshape(TOKENS, HEADS, DV)
    normalized = numerators * lax.rsqrt(lax.optimization_barrier(jnp.mean(numerators * numerators, axis=-1, keepdims=True)) + epsilon)
    cell_rows = (normalized.reshape(TOKENS, HV) * head_norm_gain * jax.nn.sigmoid(output_gate_preact.astype(jnp.float32))).astype(jnp.bfloat16)

    def finish(segment):
        cell_block, residual_block = segment
        mixed_rows = (residual_block.astype(jnp.float32) + grouped_product(cell_block, cell_output_weight, N_TP)).astype(jnp.bfloat16)
        mixed_float = mixed_rows.astype(jnp.float32)
        normed = (mixed_float * lax.rsqrt(lax.optimization_barrier(jnp.mean(mixed_float * mixed_float, axis=-1, keepdims=True)) + epsilon) * feedforward_norm_gain).astype(jnp.bfloat16)
        gate_proj = jnp.dot(normed, gate_projection_weight, preferred_element_type=jnp.float32)
        up_proj = jnp.dot(normed, up_projection_weight, preferred_element_type=jnp.float32)
        hidden = (jax.nn.silu(gate_proj) * up_proj).astype(jnp.bfloat16)
        return (mixed_float + grouped_product(hidden, down_projection_weight, N_TP)).astype(jnp.bfloat16)
    outputs = lax.map(finish, (cell_rows.reshape(TOKENS // TOK_DEV, TOK_DEV, HV), residual.reshape(TOKENS // TOK_DEV, TOK_DEV, D)))
    return outputs.reshape(TOKENS, D)
```

```python
import jax
import jax.numpy as jnp
from jax import lax
from jax.experimental import pallas as pl
from jax.experimental.pallas import tpu as pltpu
from jax.sharding import PartitionSpec as P


DQK = 64
DV = 128
BLOCK = 128


epsilon = 1e-06
lowest = -1e30


def swap(value, axis, bit):
    return lax.ppermute(value, axis, [(i, i ^ bit) for i in range(lax.axis_size(axis))])


def bits_below(size):
    return [1 << k for k in range(size.bit_length() - 1)]


def pack_state(state):
    value, top, total = state
    heads, _, width = value.shape
    extra = jnp.stack([top, total], axis=1)[:, :, None]
    extra = jnp.broadcast_to(extra, (heads, 2, width))
    return jnp.concatenate([value, extra, jnp.zeros((heads, 6, width), jnp.float32)], axis=1)


def unpack_state(packed):
    depth = packed.shape[1] - 8
    return (packed[:, :depth], packed[:, depth, 0], packed[:, depth + 1, 0])


def choose(condition, first, second):
    return jax.tree.map(lambda a, b: jnp.where(condition, a, b), first, second)


def prefix_of(state, axis, blank):
    here = lax.axis_index(axis)
    before, whole = blank, state
    for bit in bits_below(lax.axis_size(axis)):
        other = unpack_state(swap(pack_state(whole), axis, bit))
        upper = (here & bit) != 0
        before = choose(upper, merge_states(other, before), before)
        whole = merge_states(choose(upper, other, whole), choose(upper, whole, other))
    return before


def spread(piece, bits):
    held = [(0, piece)]
    for bit in bits:
        held = held + [(mask | bit, swap(value, "sp", bit)) for mask, value in held]
    return held


def merge_states(earlier, later):
    state_one, top_one, total_one = earlier
    state_two, top_two, total_two = later
    top_new = jnp.maximum(total_two + top_one, top_two)
    scale_one = jnp.exp(total_two + top_one - top_new)
    scale_two = jnp.exp(top_two - top_new)
    state_new = scale_one[..., None, None] * state_one + scale_two[..., None, None] * state_two
    return (state_new, top_new, total_one + total_two)


def add_halves(kept, sent, axis, bit):
    received = swap(sent.astype(jnp.bfloat16), axis, bit)
    return kept.astype(jnp.float32) + received.astype(jnp.float32)


def layer(
    queries,
    key_head_rows,
    value_head_rows,
    output_gate_preact,
    log_input_gate,
    forget_gate_preact,
    extra_log_decay,
    head_norm_gain,
    residual,
    cell_output_weight,
    feedforward_norm_gain,
    gate_projection_weight,
    up_projection_weight,
    down_projection_weight,
):
    size = lax.axis_size("sp")
    here = lax.axis_index("sp")
    place = lax.axis_index("tp")
    tp_bits = bits_below(lax.axis_size("tp"))
    sp_bits = bits_below(size)
    share = sp_bits[len(sp_bits) // 2]
    others = [bit for bit in reversed(sp_bits) if bit != share]
    half = gate_projection_weight.shape[1] // 2
    upper = (here & share) != 0

    def halves(first, second):
        return jnp.where(upper, second, first), jnp.where(upper, first, second)

    def columns_of(weight):
        mine, theirs = halves(weight[:, :half], weight[:, half:])
        return jnp.concatenate(halves(mine, swap(theirs, "sp", share)), axis=0)

    def rows_of(weight):
        mine, theirs = halves(weight[:half], weight[half:])
        return jnp.concatenate(halves(mine, swap(theirs, "sp", share)), axis=1)

    gate_pair = columns_of(gate_projection_weight)
    up_pair = columns_of(up_projection_weight)
    down_pair = rows_of(down_projection_weight)
    gate_pieces = spread(gate_pair, others)
    up_pieces = spread(up_pair, others)
    down_pieces = spread(down_pair, others)

    tokens_here = queries.shape[0]
    heads_here = queries.shape[1] // DQK
    scale = DQK ** (-0.5)
    query_rows = queries.reshape(tokens_here, heads_here, DQK)
    key_rows = key_head_rows.reshape(tokens_here, heads_here, DQK)
    value_rows = value_head_rows.reshape(tokens_here, heads_here, DV)

    log_forget = jax.nn.log_sigmoid(forget_gate_preact) + extra_log_decay
    in_block = jnp.cumsum(log_forget.reshape(heads_here, -1, BLOCK), axis=-1)
    block_ends = jnp.cumsum(in_block[..., -1], axis=-1)
    block_starts = jnp.pad(block_ends[:, :-1], ((0, 0), (1, 0)))
    running = (in_block + block_starts[..., None]).reshape(heads_here, tokens_here)
    total = block_ends[:, -1]
    to_end = total[:, None] - running + log_input_gate
    top = jnp.max(to_end, axis=-1)
    factor = jnp.exp(to_end - top[:, None]) * scale
    weighted = (key_rows * factor.T[:, :, None]).astype(jnp.bfloat16)
    state = jnp.einsum("shd,she->hde", weighted, value_rows, preferred_element_type=jnp.float32)
    blank_state = (
        jnp.zeros((heads_here, DQK, DV), jnp.float32),
        jnp.full((heads_here,), lowest, jnp.float32),
        jnp.zeros((heads_here,), jnp.float32),
    )
    carried_state, carried_top, _ = prefix_of((state, top, total), "sp", blank_state)

    gain = log_input_gate - running
    causal = jnp.arange(tokens_here)[:, None] >= jnp.arange(tokens_here)[None, :]
    gain_seen = jnp.where(causal, gain[:, None, :], -jnp.inf)
    own_top = jnp.max(gain_seen, axis=-1)
    scores = (
        jnp.einsum("thd,shd->hts", query_rows, key_rows, preferred_element_type=jnp.float32)
        * scale
    )
    weights = (scores * jnp.exp(gain_seen - own_top[..., None])).astype(jnp.bfloat16)
    within = jnp.einsum("hts,she->hte", weights, value_rows, preferred_element_type=jnp.float32)
    across = jnp.einsum(
        "thd,hde->hte",
        query_rows.astype(jnp.float32),
        carried_state,
        precision=lax.Precision.HIGHEST,
    )
    row_top = jnp.maximum(carried_top[:, None], own_top)
    numerators = (
        jnp.exp(carried_top[:, None] - row_top)[..., None] * across
        + jnp.exp(own_top - row_top)[..., None] * within
    )
    normalized = numerators * lax.rsqrt(
        jnp.mean(numerators * numerators, axis=-1, keepdims=True) + epsilon
    )
    cell_rows = (
        normalized.transpose(1, 0, 2).reshape(tokens_here, heads_here * DV)
        * head_norm_gain
        * jax.nn.sigmoid(output_gate_preact.astype(jnp.float32))
    ).astype(jnp.bfloat16)

    tp_size = lax.axis_size("tp")
    rows = tokens_here // tp_size
    order = [0]
    for bit in reversed(tp_bits):
        order = order + [mask | bit for mask in order]

    def cell_product(some):
        left = jnp.concatenate(
            [lax.dynamic_slice_in_dim(cell_rows, (place ^ m) * rows, rows, 0) for m in some], axis=0
        )
        product = jnp.dot(left, cell_output_weight, preferred_element_type=jnp.float32)
        return product.astype(jnp.bfloat16)

    far = cell_product(order[tp_size // 2 :])
    projected = add_halves(cell_product(order[: tp_size // 2]), far, "tp", tp_bits[0])
    for bit in tp_bits[1:]:
        kept, sent = jnp.split(projected, 2, axis=0)
        projected = add_halves(kept.astype(jnp.bfloat16), sent, "tp", bit)
    mixed_float = (
        (residual.astype(jnp.float32) + projected).astype(jnp.bfloat16).astype(jnp.float32)
    )
    normed = (
        mixed_float
        * lax.rsqrt(jnp.mean(mixed_float * mixed_float, axis=-1, keepdims=True) + epsilon)
        * feedforward_norm_gain
    ).astype(jnp.bfloat16)

    early = [mask for mask, _ in gate_pieces if not mask & others[0]]
    late = [mask for mask, _ in gate_pieces if mask & others[0]]

    def joined(pieces, masks):
        return jnp.concatenate([dict(pieces)[mask] for mask in masks], axis=0)

    gate_early, up_early = joined(gate_pieces, early), joined(up_pieces, early)
    gate_late, up_late = joined(gate_pieces, late), joined(up_pieces, late)
    normed, gate_early = lax.optimization_barrier((normed, gate_early))

    width = gate_projection_weight.shape[0]
    base = here & ~share
    normed = jnp.concatenate(
        [
            lax.dynamic_slice_in_dim(normed, ((base ^ mask) | low) * width, width, 1)
            for mask in early + late
            for low in (0, share)
        ],
        axis=1,
    )
    paired = swap(normed, "sp", share)
    paired, up_early = lax.optimization_barrier((paired, up_early))
    held = [normed, paired]
    for bit in reversed(tp_bits[1:]):
        held = held + [swap(v, "tp", bit) for v in held]
    near_rows = jnp.concatenate(held, axis=0)
    far_rows = swap(near_rows, "tp", tp_bits[0])

    def product_of(left, first, second):
        split = first.shape[0]
        return jnp.dot(left[:, :split], first, preferred_element_type=jnp.float32) + jnp.dot(
            left[:, split:], second, preferred_element_type=jnp.float32
        )

    def hidden_of(left):
        gate_proj = product_of(left, gate_early, gate_late)
        up_proj = product_of(left, up_early, up_late)
        return (jax.nn.silu(gate_proj) * up_proj).astype(jnp.bfloat16)

    hidden_near = hidden_of(near_rows)
    hidden_far = hidden_of(far_rows)

    def down_product(left, piece):
        product = jnp.dot(left, piece, preferred_element_type=jnp.float32)
        return product.astype(jnp.bfloat16)

    def sum_pair(partial):
        parts = partial.reshape(-1, 2, rows, partial.shape[1])
        kept, sent = (parts[:, k].reshape(-1, partial.shape[1]) for k in (0, 1))
        return add_halves(kept, sent, "sp", share)

    def sum_rest(partial):
        for bit in tp_bits[1:]:
            kept, sent = jnp.split(partial.astype(jnp.bfloat16), 2, axis=0)
            partial = add_halves(kept, sent, "tp", bit)
        return partial

    blocks = {}
    for k, (mask, piece) in enumerate(sorted(down_pieces, key=lambda entry: entry[0])):
        far = down_product(hidden_far, piece)
        near = down_product(hidden_near, piece)
        partial = add_halves(near, far, "tp", tp_bits[0]).astype(jnp.bfloat16)
        if k % 2:
            blocks[mask] = sum_rest(sum_pair(partial))
        else:
            blocks[mask] = sum_pair(sum_rest(partial).astype(jnp.bfloat16))
    lows = share.bit_length() - 1
    masks = sorted(blocks)
    relative = jnp.concatenate([blocks[mask] for mask in masks], axis=1)
    columns = []
    for block in range(size):
        mask = (block ^ here) & ~share
        position = ((mask >> (lows + 1)) << lows) | (mask & (share - 1))
        start = (2 * position + ((block >> lows) & 1)) * width
        columns.append(lax.dynamic_slice_in_dim(relative, start, width, 1))
    summed = jnp.concatenate(columns, axis=1)
    return (mixed_float + summed).astype(jnp.bfloat16)


def per_device(*arrays):
    return layer(*arrays)


MESH = pl.DeviceIdType.MESH
SIDE = 2
LINE = 4
LANES = 128
VMEM_BYTES = 64 * 1024 * 1024
A0, A1, B1, B0 = range(LINE)
F32, BF16 = jnp.float32, jnp.bfloat16
EXACT = lax.Precision.HIGHEST
NT = (((1,), (1,)), ((), ()))
TN = (((0,), (0,)), ((), ()))


def fits(mesh):
    return mesh.shape["sp"] == LINE * SIDE and mesh.shape["tp"] == SIDE * 2


def cell_kernel(
    q_ref,
    k_ref,
    v_ref,
    li_ref,
    fg_ref,
    ed_ref,
    hng_ref,
    fng_ref,
    og_hbm,
    res_hbm,
    cw_hbm,
    gate_hbm,
    up_hbm,
    down_hbm,
    out_ref,
    og_ref,
    res_ref,
    cw_ref,
    tile_ref,
    wgu_ref,
    wd_ref,
    pgu_ref,
    pd_ref,
    fgu_ref,
    fd_ref,
    gain_ref,
    fac_ref,
    wi_ref,
    ot_ref,
    cell_ref,
    st_ref,
    before_ref,
    tops_ref,
    opc_send,
    opc_recv,
    op_keep,
    opy_send,
    opy_recv,
    mixed_ref,
    x_ref,
    h_ref,
    rc_send,
    rc_recv,
    r_keep,
    ry_send,
    ry_recv,
    rz_send,
    rz_recv,
    load_sem,
    pack_sem,
    zs_sem,
    zr_sem,
    xs_sem,
    xr_sem,
    fr_sem,
    cs_sem,
    st_ss,
    st_rs,
    op_ss,
    op_rs,
    ag_ss,
    ag_rs,
    rs_ss,
    rs_rs,
):
    sp = lax.axis_index("sp")
    tp = lax.axis_index("tp")
    z, x = lax.div(sp, SIDE), lax.rem(sp, SIDE)
    y, c = lax.div(tp, 2), lax.rem(tp, 2)
    h, low = lax.div(z, 2), lax.rem(z, 2)
    b = lax.rem(h + low, 2)
    is_mid, is_end = b == 1, b == 0
    upper = h == 1
    lower = h == 0
    to_x = (z * SIDE + (1 - x), tp)
    to_y = (sp, (1 - y) * 2 + c)
    to_c = (sp, y * 2 + (1 - c))
    to_pair = ((2 * h + (1 - low)) * SIDE + x, tp)
    to_cross = ((LINE - 1 - z) * SIDE + x, tp)
    z_of = ((LINE - 1) * h, 1 + h, 2 - h, (LINE - 1) * (1 - h))
    src = tuple(zz * SIDE + x for zz in z_of)
    src_x = tuple(zz * SIDE + (1 - x) for zz in z_of)

    tokens = q_ref.shape[0]
    heads = q_ref.shape[1] // DQK
    width = gate_hbm.shape[0]
    tiles = gate_hbm.shape[1] // LANES
    whole = tiles // 2
    half = pd_ref.shape[0]
    rows = res_ref.shape[0]
    part = rows // 2
    model = res_ref.shape[1]
    blocks = tokens // BLOCK
    scale = DQK ** (-0.5)

    def remote(source, target, ssem, rsem, device):
        return pltpu.make_async_remote_copy(
            src_ref=source,
            dst_ref=target,
            send_sem=ssem,
            recv_sem=rsem,
            device_id=device,
            device_id_type=MESH,
        )

    def got(target, rsem):
        remote(target, target, rsem, rsem, to_x).wait_recv()

    loads = (
        pltpu.make_async_copy(og_hbm, og_ref, load_sem.at[0]),
        pltpu.make_async_copy(res_hbm, res_ref, load_sem.at[1]),
        pltpu.make_async_copy(cw_hbm, cw_ref, load_sem.at[2]),
    )

    def rows_at(index, start=0, count=None):
        count = width if count is None else count
        return pl.ds(pl.multiple_of(index * width + start, LANES), count)

    own = z * SIDE + x
    packs = []

    def pack(source, target):
        packs.append(pltpu.make_async_copy(source, target, pack_sem.at[len(packs)]))

    pack(gate_hbm.at[:, whole * LANES : (whole + 1) * LANES], tile_ref.at[0])
    pack(up_hbm.at[:, whole * LANES : (whole + 1) * LANES], tile_ref.at[1])
    for mine in (0, 1):
        side = b if mine == 0 else 1 - b
        for i in range(whole):
            lanes = pl.ds(pl.multiple_of((side * (whole + 1) + i) * LANES, LANES), LANES)
            for k, weight in enumerate((gate_hbm, up_hbm)):
                put = pl.ds((2 * i + k) * LANES, LANES)
                if mine == 0:
                    pack(weight.at[:, lanes], wgu_ref.at[rows_at(own), put])
                else:
                    pack(weight.at[:, lanes], pgu_ref.at[:, put])
        main = pl.ds(pl.multiple_of(side * (whole + 1) * LANES, LANES), whole * LANES)
        rest = pl.ds(
            pl.multiple_of(whole * LANES + side * (LANES // 2), LANES // 2), LANES // 2
        )
        for at, put in ((main, slice(0, whole * LANES)), (rest, slice(whole * LANES, half))):
            if mine == 0:
                pack(down_hbm.at[at], wd_ref.at[own, put])
            else:
                pack(down_hbm.at[at], pd_ref.at[put])
    for copy in packs:
        copy.start()
    for copy in loads:
        copy.start()

    barrier = pltpu.get_barrier_semaphore()
    for device in (to_x, to_y, to_c, to_pair):
        pl.semaphore_signal(barrier, inc=1, device_id=device, device_id_type=MESH)

    @pl.when(is_mid)
    def _():
        pl.semaphore_signal(barrier, inc=1, device_id=to_cross, device_id_type=MESH)

    pl.semaphore_wait(barrier, 4 + b)

    for copy in packs:
        copy.wait()
    lane = lax.broadcasted_iota(jnp.int32, (width, LANES), 1)
    left = lane < LANES // 2
    tile_g, tile_u = tile_ref[0].astype(F32), tile_ref[1].astype(F32)
    merged_end = jnp.where(left, tile_g, pltpu.roll(tile_u, LANES // 2, 1)).astype(BF16)
    merged_mid = jnp.where(left, pltpu.roll(tile_g, LANES // 2, 1), tile_u).astype(BF16)
    tail = slice(2 * whole * LANES, (2 * whole + 1) * LANES)
    ends = jnp.full((width, LANES), b, jnp.int32) == 0
    wgu_ref[rows_at(own), tail] = jnp.where(ends, merged_end, merged_mid)
    pgu_ref[:, tail] = jnp.where(ends, merged_mid, merged_end)
    wd_ref[:, half:, :] = jnp.zeros((LINE * SIDE, wd_ref.shape[1] - half, width), BF16)

    def chunk_gu(ref, t, index=None):
        cut = width // 2
        if index is None:
            return ref.at[pl.ds(t * cut, cut)]
        return ref.at[rows_at(index, t * cut, cut)]

    def wanted(index, t):
        if t < 2:
            return chunk_gu(wgu_ref, t, index)
        return wd_ref.at[index, 0:half]

    def other(t):
        return chunk_gu(pgu_ref, t) if t < 2 else pd_ref

    def passing(k, t):
        return chunk_gu(fgu_ref.at[k], t) if t < 2 else fd_ref.at[k]

    def x_copy(j, t):
        return remote(
            wanted(src[j], t), wanted(src[j], t), xs_sem.at[j, t], xr_sem.at[j, t], to_x
        )

    def pair_from_end(kind, t):
        if kind == "M":
            return remote(other(t), wanted(own, t), zs_sem.at[0, t], zr_sem.at[A0, t], to_pair)
        return remote(wanted(own, t), passing(0, t), zs_sem.at[1, t], fr_sem.at[0, t], to_pair)

    def pair_from_mid(kind, t):
        j = {"o": A1, "c": B1, "q": B0}[kind]
        source = {"o": other, "c": lambda t: passing(1, t), "q": lambda t: passing(2, t)}[kind](t)
        return remote(source, wanted(src[j], t), zs_sem.at[j - 1, t], zr_sem.at[j, t], to_pair)

    def cross(kind, t):
        if kind == "Eo":
            return remote(other(t), passing(1, t), cs_sem.at[0, t], fr_sem.at[1, t], to_cross)
        if kind == "Mo":
            return remote(
                wanted(own, t), wanted(own, t), cs_sem.at[1, t], zr_sem.at[B1, t], to_cross
            )
        if kind == "Ep":
            return remote(passing(0, t), passing(2, t), cs_sem.at[2, t], fr_sem.at[2, t], to_cross)
        return remote(
            wanted(src[A0], t), wanted(src[A0], t), cs_sem.at[3, t], zr_sem.at[B0, t], to_cross
        )

    def when(condition, *copies):
        @pl.when(condition)
        def _():
            for make in copies:
                make().start()

    def x_own(t):
        when(is_end, lambda: x_copy(A0, t))
        when(is_mid, lambda: x_copy(A1, t))

    def arrived(j, t):
        got(wanted(src[j], t), zr_sem.at[j, t])

    def arrived_x(j, t):
        got(wanted(src_x[j], t), xr_sem.at[j, t])

    def to_pass(k, t):
        got(passing(k, t), fr_sem.at[k, t])

    when(is_end, lambda: pair_from_end("M", 0))
    when(is_mid, lambda: cross("Eo", 0), lambda: pair_from_mid("o", 0))
    x_own(0)
    when(
        is_end & upper,
        lambda: pair_from_end("E", 0),
        lambda: pair_from_end("M", 1),
        lambda: pair_from_end("E", 1),
    )
    when(
        is_mid & upper,
        lambda: cross("Mo", 0),
        lambda: cross("Eo", 1),
        lambda: cross("Mo", 1),
    )
    when(is_mid & lower, lambda: pair_from_mid("o", 1))

    upto = (
        lax.broadcasted_iota(jnp.int32, (BLOCK, BLOCK), 0)
        <= lax.broadcasted_iota(jnp.int32, (BLOCK, BLOCK), 1)
    ).astype(F32)
    same = (
        lax.broadcasted_iota(jnp.int32, (BLOCK, BLOCK), 0)
        == lax.broadcasted_iota(jnp.int32, (BLOCK, BLOCK), 1)
    ).astype(F32)
    forget = fg_ref[...]
    log_forget = jnp.minimum(forget, 0.0) - jnp.log1p(jnp.exp(-jnp.abs(forget))) + ed_ref[...]
    offset = jnp.zeros((heads, 1), F32)
    running = []
    for i in range(blocks):
        inside = jnp.dot(
            log_forget[:, i * BLOCK : (i + 1) * BLOCK],
            upto,
            precision=EXACT,
            preferred_element_type=F32,
        )
        running.append(inside + offset)
        offset = offset + inside[:, BLOCK - 1 : BLOCK]
    total = offset
    running = jnp.concatenate(running, axis=1)
    gain = li_ref[...] - running
    for k in range(heads):
        gain_ref[k] = gain[k : k + 1, :]
    to_end = total + gain
    top = jnp.max(to_end, axis=1, keepdims=True)
    factor = jnp.exp(to_end - top) * scale
    head_lane = lax.broadcasted_iota(jnp.int32, (BLOCK, LANES), 1) < DQK
    for i in range(blocks):
        at = slice(i * BLOCK, (i + 1) * BLOCK)
        columns = lax.dot_general(
            same, factor[:, at], NT, precision=EXACT, preferred_element_type=F32
        )
        for p in range(heads // 2):
            pair = slice(p * LANES, (p + 1) * LANES)
            by_lane = jnp.where(
                head_lane, columns[:, 2 * p : 2 * p + 1], columns[:, 2 * p + 1 : 2 * p + 2]
            )
            fac_ref[at, pair] = (k_ref[at, pair].astype(F32) * by_lane).astype(BF16)
    head_row = lax.broadcasted_iota(jnp.int32, (LANES, LANES), 0) < DQK
    depth = heads // 2 * LANES

    def write_state(slot, value, top_rows, total_rows):
        for p in range(heads // 2):
            st_ref[slot, p * LANES : (p + 1) * LANES, :] = value[p]
        st_ref[slot, depth : depth + heads, :] = top_rows
        st_ref[slot, depth + heads : depth + 2 * heads, :] = total_rows

    def read_state(slot):
        value = [st_ref[slot, p * LANES : (p + 1) * LANES, :] for p in range(heads // 2)]
        return (
            value,
            st_ref[slot, depth : depth + heads, :],
            st_ref[slot, depth + heads : depth + 2 * heads, :],
        )

    def merge(earlier, later):
        value_one, top_one, total_one = earlier
        value_two, top_two, total_two = later
        top_new = jnp.maximum(total_two + top_one, top_two)
        scale_one = jnp.exp(total_two + top_one - top_new)
        scale_two = jnp.exp(top_two - top_new)

        def by_row(scales, p):
            return jnp.where(
                head_row, scales[2 * p : 2 * p + 1, :], scales[2 * p + 1 : 2 * p + 2, :]
            )

        value = [
            by_row(scale_one, p) * value_one[p] + by_row(scale_two, p) * value_two[p]
            for p in range(heads // 2)
        ]
        return value, top_new, total_one + total_two

    value = []
    for p in range(heads // 2):
        pair = slice(p * LANES, (p + 1) * LANES)
        first, second = (
            lax.dot_general(
                fac_ref[:, pair],
                v_ref[:, (2 * p + k) * DV : (2 * p + k + 1) * DV],
                TN,
                preferred_element_type=F32,
            )
            for k in (0, 1)
        )
        value.append(jnp.where(head_row, first, second))
    write_state(
        0, value, jnp.broadcast_to(top, (heads, LANES)), jnp.broadcast_to(total, (heads, LANES))
    )
    swap_state = remote(st_ref.at[0], st_ref.at[1], st_ss.at[0], st_rs.at[0], to_x)
    swap_state.start()
    x_own(1)

    def within(head):
        lanes = pl.ds(pl.multiple_of(lax.div(head, 2) * LANES, LANES), LANES)
        columns = pl.ds(pl.multiple_of(head * DV, DV), DV)
        mine = lax.div(lax.broadcasted_iota(jnp.int32, (BLOCK, LANES), 1), DQK) == lax.rem(head, 2)
        for i in range(blocks):
            at = slice(i * BLOCK, (i + 1) * BLOCK)
            seen = (i + 1) * BLOCK
            query = jnp.where(mine, q_ref[at, lanes], jnp.zeros((BLOCK, LANES), BF16))
            scores = lax.dot_general(
                query, k_ref[0:seen, lanes], NT, preferred_element_type=F32
            )
            causal = (
                lax.broadcasted_iota(jnp.int32, (BLOCK, seen), 0) + i * BLOCK
                >= lax.broadcasted_iota(jnp.int32, (BLOCK, seen), 1)
            )
            row = gain_ref[head, :, 0:seen]
            gain_seen = jnp.where(causal, row, -jnp.inf)
            own_top = jnp.max(gain_seen, axis=1, keepdims=True)
            weights = (scores * scale * jnp.exp(gain_seen - own_top)).astype(BF16)
            wi_ref[head, at, :] = jnp.dot(
                weights, v_ref[0:seen, columns], preferred_element_type=F32
            )
            ot_ref[head, at, :] = jnp.broadcast_to(own_top, (BLOCK, DV))

    def loop(count, body):
        def step(i, carry):
            body(i)
            return carry

        lax.fori_loop(0, count, step, 0)

    swap_state.wait_recv()
    blank = (
        [jnp.zeros((LANES, LANES), F32) for _ in range(heads // 2)],
        jnp.full((heads, LANES), lowest, F32),
        jnp.zeros((heads, LANES), F32),
    )
    is_first = x == 0

    @pl.when(is_first)
    def _():
        write_state(4, *merge(read_state(0), read_state(1)))

    @pl.when(jnp.logical_not(is_first))
    def _():
        write_state(4, *merge(read_state(1), read_state(0)))

    to_up = (jnp.minimum(z + 1, LINE - 1) * SIDE + x, tp)
    lift = remote(st_ref.at[2], st_ref.at[3], st_ss.at[1], st_rs.at[1], to_up)

    @pl.when(z == 0)
    def _():
        write_state(2, *read_state(4))
        write_state(3, *blank)
        lift.start()

    when(
        is_end & lower,
        lambda: pair_from_end("E", 0),
        lambda: pair_from_end("M", 1),
        lambda: pair_from_end("E", 1),
    )
    loop(heads // 2, within)

    @pl.when(z > 0)
    def _():
        lift.wait_recv()

    @pl.when((z > 0) & (z < LINE - 1))
    def _():
        write_state(2, *merge(read_state(3), read_state(4)))
        lift.start()

    when(
        is_mid & lower,
        lambda: cross("Mo", 0),
        lambda: cross("Eo", 1),
        lambda: cross("Mo", 1),
    )
    when(is_mid & upper, lambda: pair_from_mid("o", 1))
    loop(heads // 2, lambda i: within(i + heads // 2))

    def write_before(state):
        value, tops, _ = state
        for p in range(heads // 2):
            before_ref[p * LANES : (p + 1) * LANES, :] = value[p]
        for k in range(heads):
            tops_ref[k] = tops[k : k + 1, :]

    @pl.when(is_first)
    def _():
        write_before(read_state(3))

    @pl.when(jnp.logical_not(is_first))
    def _():
        write_before(merge(read_state(3), read_state(1)))

    loads[0].wait()

    def finish(step):
        head, i = lax.div(step, blocks), lax.rem(step, blocks)
        lanes = pl.ds(pl.multiple_of(lax.div(head, 2) * LANES, LANES), LANES)
        columns = pl.ds(pl.multiple_of(head * DV, DV), DV)
        at = pl.ds(pl.multiple_of(i * BLOCK, BLOCK), BLOCK)
        mine = lax.div(lax.broadcasted_iota(jnp.int32, (BLOCK, LANES), 1), DQK) == lax.rem(head, 2)
        query = jnp.where(mine, q_ref[at, lanes], jnp.zeros((BLOCK, LANES), BF16))
        carried = before_ref[pl.ds(pl.multiple_of(lax.div(head, 2) * LANES, LANES), LANES), :]
        carried_high = carried.astype(BF16)
        carried_low = (carried - carried_high.astype(F32)).astype(BF16)
        across = jnp.dot(query, carried_high, preferred_element_type=F32) + jnp.dot(
            query, carried_low, preferred_element_type=F32
        )
        carried_top = tops_ref[head]
        own_top = ot_ref[head, at, :]
        row_top = jnp.maximum(carried_top, own_top)
        numerator = (
            jnp.exp(carried_top - row_top) * across
            + jnp.exp(own_top - row_top) * wi_ref[head, at, :]
        )
        spread_of = jnp.mean(numerator * numerator, axis=1, keepdims=True)
        gate = og_ref[at, columns].astype(F32)
        cell = (
            numerator
            * lax.rsqrt(spread_of + epsilon)
            * hng_ref[:, columns]
            / (1.0 + jnp.exp(-gate))
        )
        cell_ref[at, columns] = cell.astype(BF16)

    loop(heads * blocks, finish)

    @pl.when(is_mid)
    def _():
        arrived(A0, 0)
        x_copy(A0, 0).start()
        to_pass(1, 0)
        pair_from_mid("c", 0).start()
        to_pass(0, 0)
        cross("Ep", 0).start()
        cross("Mp", 0).start()

    @pl.when(is_end)
    def _():
        arrived(A1, 0)
        x_copy(A1, 0).start()

    loads[1].wait()
    loads[2].wait()

    def cell_part(yy, cc, r):
        start = pl.multiple_of((yy * 2 + cc) * rows + r * part, 16)
        return cell_ref[pl.ds(start, part), :]

    op_core = [
        remote(opc_send.at[r], opc_recv.at[r], op_ss.at[0, r], op_rs.at[0, r], to_c)
        for r in (0, 1)
    ]
    op_y = [
        remote(opy_send.at[r], opy_recv.at[r], op_ss.at[1, r], op_rs.at[1, r], to_y)
        for r in (0, 1)
    ]
    cut = model // 4

    def product(cc, r, put):
        left = jnp.concatenate([cell_part(1 - y, cc, r), cell_part(y, cc, r)], axis=0)

        def body(n):
            lanes = pl.ds(pl.multiple_of(n * cut, cut), cut)
            put(lanes, jnp.dot(left, cw_ref[:, lanes], preferred_element_type=F32))

        loop(4, body)

    def ag_copy(kind, slot, r):
        bit, device = {"z": (1, to_pair), "y": (2, to_y), "c": (4, to_c)}[kind]
        k = {"z": 0, "y": 1, "c": 3}[kind] + slot
        there = slot + bit
        return remote(
            x_ref.at[pl.ds(slot * rows + r * part, part)],
            x_ref.at[pl.ds(there * rows + r * part, part)],
            ag_ss.at[k, r],
            ag_rs.at[k, r],
            device,
        )

    def ag_got(kind, slot, r):
        bit = {"z": 1, "y": 2, "c": 4}[kind]
        k = {"z": 0, "y": 1, "c": 3}[kind] + slot
        got(x_ref.at[pl.ds((slot + bit) * rows + r * part, part)], ag_rs.at[k, r])

    for r in (0, 1):

        def put_far(lanes, value):
            opc_send[r, :, lanes] = value.astype(BF16)

        def put_near(lanes, value):
            op_keep[r, :, lanes] = value

        product(1 - c, r, put_far)
        op_core[r].start()
        product(c, r, put_near)
        op_core[r].wait_recv()
        opy_send[r] = (op_keep[r, 0:part, :] + opc_recv[r, 0:part, :].astype(F32)).astype(BF16)
        op_y[r].start()
        op_keep[r, part : 2 * part, :] += opc_recv[r, part : 2 * part, :].astype(F32)

    @pl.when(is_mid)
    def _():
        to_pass(1, 1)
        pair_from_mid("c", 1).start()
        arrived(A0, 1)
        x_copy(A0, 1).start()
        to_pass(0, 1)
        cross("Ep", 1).start()
        cross("Mp", 1).start()

    @pl.when(is_end)
    def _():
        arrived(A1, 1)
        x_copy(A1, 1).start()

    for r in (0, 1):
        op_y[r].wait_recv()
        at = slice(r * part, (r + 1) * part)
        mixed = (
            res_ref[at, :].astype(F32)
            + (op_keep[r, part : 2 * part, :] + opy_recv[r].astype(F32))
        ).astype(BF16)
        mixed_ref[at, :] = mixed
        mixed_float = mixed.astype(F32)
        spread_of = jnp.mean(mixed_float * mixed_float, axis=1, keepdims=True)
        x_ref[at, :] = (mixed_float * lax.rsqrt(spread_of + epsilon) * fng_ref[...]).astype(BF16)
        ag_copy("z", 0, r).start()
        ag_copy("y", 0, r).start()
        ag_copy("c", 0, r).start()

    @pl.when(is_mid)
    def _():
        arrived(B1, 0)
        x_copy(B1, 0).start()
        arrived(B1, 1)
        x_copy(B1, 1).start()
        cross("Eo", 2).start()
        cross("Mo", 2).start()
        pair_from_mid("o", 2).start()

    @pl.when(is_end)
    def _():
        pair_from_end("M", 2).start()
        pair_from_end("E", 2).start()
        arrived(B1, 0)
        x_copy(B1, 0).start()
        arrived(B1, 1)
        x_copy(B1, 1).start()

    x_own(2)
    for r in (0, 1):
        ag_got("z", 0, r)
        ag_copy("y", 1, r).start()
        ag_copy("c", 1, r).start()
    for r in (0, 1):
        ag_got("y", 0, r)
        ag_copy("c", 2, r).start()

    @pl.when(is_mid)
    def _():
        to_pass(2, 0)
        pair_from_mid("q", 0).start()
        arrived(B0, 0)
        x_copy(B0, 0).start()
        arrived(A0, 2)
        to_pass(0, 2)
        cross("Ep", 2).start()
        cross("Mp", 2).start()
        to_pass(2, 1)
        pair_from_mid("q", 1).start()
        arrived(B0, 1)
        x_copy(B0, 1).start()
        x_copy(A0, 2).start()

    @pl.when(is_end)
    def _():
        arrived(B0, 0)
        x_copy(B0, 0).start()
        arrived(A1, 2)
        x_copy(A1, 2).start()
        arrived(B0, 1)
        x_copy(B0, 1).start()

    for r in (0, 1):
        ag_got("y", 1, r)
        ag_copy("c", 3, r).start()
    for slot in range(4):
        for r in (0, 1):
            ag_got("c", slot, r)
    for j in range(LINE):
        arrived_x(j, 0)
        arrived_x(j, 1)

    group = 2 * rows
    groups = x_ref.shape[0] // group

    def gated(value, gate):
        return (value / (1.0 + jnp.exp(-value)) * gate).astype(BF16)

    def hidden(step):
        m, i = lax.rem(step, groups), lax.div(step, groups)
        at = pl.ds(pl.multiple_of(m * group, 16), group)
        both = jnp.dot(
            x_ref[at, :],
            wgu_ref[:, pl.ds(pl.multiple_of(i * 2 * LANES, 2 * LANES), 2 * LANES)],
            preferred_element_type=F32,
        )
        h_ref[at, pl.ds(pl.multiple_of(i * LANES, LANES), LANES)] = gated(
            both[:, :LANES], both[:, LANES:]
        )

    def hidden_rest(m):
        at = pl.ds(pl.multiple_of(m * group, 16), group)
        both = jnp.dot(x_ref[at, :], wgu_ref[:, tail], preferred_element_type=F32)
        value = gated(both, pltpu.roll(both, LANES // 2, 1))
        inside = lax.broadcasted_iota(jnp.int32, (group, LANES), 1) < LANES // 2
        h_ref[at, whole * LANES :] = jnp.where(inside, value, jnp.zeros_like(value))

    loop(groups * whole, hidden)
    loop(groups, hidden_rest)

    @pl.when(is_mid)
    def _():
        to_pass(1, 2)
        pair_from_mid("c", 2).start()

    order = ((A0, 0), (A1, 0), (A0, 1), (A1, 1), (B1, 0), (B1, 1), (B0, 0), (B0, 1))
    count = len(order)
    kept = x_ref.shape[0] // 2

    def source_of(k):
        j, far = order[k]
        return (src_x if far else src)[j]

    core_copy = [
        remote(rc_send.at[k], rc_recv.at[k], rs_ss.at[0, k], rs_rs.at[0, k], to_c)
        for k in range(count)
    ]
    y_copy = [
        remote(ry_send.at[k], ry_recv.at[k], rs_ss.at[1, k], rs_rs.at[1, k], to_y)
        for k in range(count)
    ]
    z_copy = [
        remote(rz_send.at[k], rz_recv.at[k], rs_ss.at[2, k], rs_rs.at[2, k], to_pair)
        for k in range(count)
    ]

    def need(k):
        j, far = order[k]
        if far:
            arrived_x(j, 2)
        elif j == A0:
            pass
        elif j == A1:
            pass
        else:
            arrived(j, 2)
            x_copy(j, 2).start()

    def stage_product(k):
        index = source_of(k)

        def far_rows(m):
            at = pl.ds(pl.multiple_of(m * group, 16), group)
            there = pl.ds(pl.multiple_of(kept + m * group, 16), group)
            rc_send[k, at, :] = jnp.dot(
                h_ref[there, :], wd_ref[index], preferred_element_type=F32
            ).astype(BF16)

        def near_rows(m):
            at = pl.ds(pl.multiple_of(m * group, 16), group)
            r_keep[k, at, :] = jnp.dot(h_ref[at, :], wd_ref[index], preferred_element_type=F32)

        loop(kept // group, far_rows)
        core_copy[k].start()
        loop(kept // group, near_rows)

    def stage_y(k):
        core_copy[k].wait_recv()
        mid_row = kept // 2
        ry_send[k] = (r_keep[k, mid_row:, :] + rc_recv[k, mid_row:, :].astype(F32)).astype(BF16)
        y_copy[k].start()
        r_keep[k, 0:mid_row, :] += rc_recv[k, 0:mid_row, :].astype(F32)

    def stage_z(k):
        y_copy[k].wait_recv()
        rz_send[k] = (r_keep[k, rows : 2 * rows, :] + ry_recv[k, rows:, :].astype(F32)).astype(BF16)
        z_copy[k].start()
        r_keep[k, 0:rows, :] += ry_recv[k, 0:rows, :].astype(F32)

    def stage_out(k):
        z_copy[k].wait_recv()
        lanes = pl.ds(pl.multiple_of(source_of(k) * width, width), width)
        out_ref[:, lanes] = (
            mixed_ref[:, lanes].astype(F32) + (r_keep[k, 0:rows, :] + rz_recv[k].astype(F32))
        ).astype(BF16)

    for step in range(count + 3):
        if step < count:
            need(step)
            stage_product(step)
        if step == 5:

            @pl.when(is_mid)
            def _():
                to_pass(2, 2)
                pair_from_mid("q", 2).start()

        if 0 <= step - 1 < count:
            stage_y(step - 1)
        if 0 <= step - 2 < count:
            stage_z(step - 2)
        if 0 <= step - 3 < count:
            stage_out(step - 3)

    for j in range(LINE):
        for t in range(3):
            x_copy(j, t).wait_send()
    for t in range(3):

        @pl.when(is_end)
        def _():
            pair_from_end("M", t).wait_send()
            pair_from_end("E", t).wait_send()

        @pl.when(is_mid)
        def _():
            for kind in ("o", "c", "q"):
                pair_from_mid(kind, t).wait_send()
            for kind in ("Eo", "Mo", "Ep", "Mp"):
                cross(kind, t).wait_send()

    swap_state.wait_send()

    @pl.when(z < LINE - 1)
    def _():
        lift.wait_send()

    for r in (0, 1):
        op_core[r].wait_send()
        op_y[r].wait_send()
        ag_copy("z", 0, r).wait_send()
        for slot in range(2):
            ag_copy("y", slot, r).wait_send()
        for slot in range(4):
            ag_copy("c", slot, r).wait_send()
    for k in range(count):
        core_copy[k].wait_send()
        y_copy[k].wait_send()
        z_copy[k].wait_send()


def layer_in_one_kernel(
    queries,
    key_head_rows,
    value_head_rows,
    output_gate_preact,
    log_input_gate,
    forget_gate_preact,
    extra_log_decay,
    head_norm_gain,
    residual,
    cell_output_weight,
    feedforward_norm_gain,
    gate_projection_weight,
    up_projection_weight,
    down_projection_weight,
):
    tokens, values = value_head_rows.shape
    heads = queries.shape[1] // DQK
    rows, model = residual.shape
    width, units = gate_projection_weight.shape
    half = units // 2
    padded = -(-half // LANES) * LANES
    part = rows // 2
    gathered = 2 * SIDE * 2 * rows
    pieces = LINE * SIDE
    state = (heads // 2 * LANES + 2 * heads, LANES)
    vmem = pl.BlockSpec(memory_space=pltpu.VMEM)
    hbm = pl.BlockSpec(memory_space=pl.ANY)

    def buf(*shape, dtype=BF16):
        return pltpu.VMEM(shape, dtype)

    sems = pltpu.SemaphoreType.DMA
    return pl.pallas_call(
        cell_kernel,
        out_shape=jax.ShapeDtypeStruct((rows, model), BF16),
        in_specs=[vmem] * 8 + [hbm] * 6,
        out_specs=vmem,
        scratch_shapes=[
            buf(tokens, values),
            buf(rows, model),
            buf(values, model),
            buf(2, width, LANES),
            buf(pieces * width, units),
            buf(pieces, padded, width),
            buf(width, units),
            buf(half, width),
            buf(3, width, units),
            buf(3, half, width),
            buf(heads, 1, tokens, dtype=F32),
            buf(tokens, heads * DQK),
            buf(heads, tokens, DV, dtype=F32),
            buf(heads, tokens, DV, dtype=F32),
            buf(tokens, values),
            buf(5, *state, dtype=F32),
            buf(heads // 2 * LANES, LANES, dtype=F32),
            buf(heads, 1, LANES, dtype=F32),
            buf(2, rows, model),
            buf(2, rows, model),
            buf(2, rows, model, dtype=F32),
            buf(2, part, model),
            buf(2, part, model),
            buf(rows, model),
            buf(gathered, model),
            buf(gathered, padded),
            buf(pieces, gathered // 2, width),
            buf(pieces, gathered // 2, width),
            buf(pieces, gathered // 2, width, dtype=F32),
            buf(pieces, gathered // 4, width),
            buf(pieces, gathered // 4, width),
            buf(pieces, rows, width),
            buf(pieces, rows, width),
            sems((3,)),
            sems((4 * (units // LANES // 2) + 6,)),
            sems((3, 3)),
            sems((LINE, 3)),
            sems((LINE, 3)),
            sems((LINE, 3)),
            sems((3, 3)),
            sems((4, 3)),
            sems((2,)),
            sems((2,)),
            sems((2, 2)),
            sems((2, 2)),
            sems((7, 2)),
            sems((7, 2)),
            sems((3, pieces)),
            sems((3, pieces)),
        ],
        compiler_params=pltpu.CompilerParams(
            collective_id=0, has_side_effects=True, vmem_limit_bytes=VMEM_BYTES
        ),
        name="layer",
    )(
        queries,
        key_head_rows,
        value_head_rows,
        log_input_gate,
        forget_gate_preact,
        extra_log_decay,
        head_norm_gain.reshape(1, -1),
        feedforward_norm_gain.reshape(1, -1),
        output_gate_preact,
        residual,
        cell_output_weight,
        gate_projection_weight,
        up_projection_weight,
        down_projection_weight,
    )


def solution(mesh):
    placed = (
        P("sp", "tp"),
        P("sp", "tp"),
        P("sp", "tp"),
        P("sp", "tp"),
        P("tp", "sp"),
        P("tp", "sp"),
        P("tp", "sp"),
        P("tp"),
        P(("sp", "tp"), None),
        P("tp", None),
        P(),
        P("sp", "tp"),
        P("sp", "tp"),
        P("tp", "sp"),
    )
    one = fits(mesh)
    return jax.shard_map(
        layer_in_one_kernel if one else per_device, mesh=mesh, in_specs=placed, out_specs=P(("sp", "tp"), None), check_vma=False
    )
```
